32 devices in a mesh: sp: 8 (over z, x), tp: 4 (over y, core).
Axes of the slice: x: 2, y: 2, z: 4, core: 2. Of those that a mesh axis runs over, the one named last changes fastest.
Arguments:
- tokens: bfloat16 [4096, 2048], P(('sp', 'tp')), may hold values from -6 to 6
- norm_gain: float32 [2048], replicated, may hold values from 0.1 to 1.9
- w_query: bfloat16 [2048, 1024], P(None, 'tp'), may hold values from -16 to 16
- w_key: bfloat16 [2048, 1024], P(None, 'tp'), may hold values from -16 to 16
- w_value: bfloat16 [2048, 1024], P(None, 'tp'), may hold values from -0.125 to 0.125
- conv_in: bfloat16 [2048, 2048], P(None, 'tp'), may hold values from -0.125 to 0.125
- conv_gate: bfloat16 [2048, 2048], P(None, 'tp'), may hold values from -0.125 to 0.125
- conv_taps: float32 [31, 2048], P(None, 'tp'), may hold values from -3.7 to 3.7
- conv_gain: float32 [2048], P('tp'), may hold values from 0.1 to 1.9
- cum_gate: float32 [16, 4096], P('tp'), may hold values from -514 to 0, as said below
- out_attn: bfloat16 [1024, 2048], P('tp'), may hold values from -0.75 to 0.75
- out_conv: bfloat16 [2048, 2048], P('tp'), may hold values from -0.125 to 0.125
Outputs:
- mixed: bfloat16 [4096, 2048], P(('sp', 'tp'))
- log_total: float32 [16, 4096], P('tp', 'sp')
The draws below stay inside these ranges and needn't reach their ends.
Inputs may be any that keep to these rules, and one draw needn't show every extreme that they name: `cum_gate`: for each head the values never rise from one position to the next and are at most 0.
All inputs are finite; a program needn't handle non-finite values.
Results may differ from the reference program's by a relative error of at most 0.014.
Values may be sent and summed in bfloat16 or wider, within the bound.
A program may use at most 128 MiB of HBM per device.

```python
import math
import jax
import jax.numpy as jnp
from jax import lax

D = 2048
HEAD_COUNT = 16
HEAD = 64
KERNEL = 31
TOK_DEV = 512
TOKEN_COUNT = 4096
ATT_WIDTH = 1024
CONV = 2048
N_SP = 8
N_TP = 4


def query_key_pair(key):
    random_split_keys = jax.random.split(jax.random.fold_in(key, 11), 3)
    fan_scale = D ** (-0.5)
    key_weight = jnp.clip(jax.random.normal(random_split_keys[0], (D, HEAD_COUNT * HEAD), jnp.float32), -6.0, 6.0) * fan_scale
    query_weight = jnp.clip(jax.random.normal(random_split_keys[2], (D, HEAD_COUNT * HEAD), jnp.float32), -6.0, 6.0) * (2.25 * fan_scale)
    return (query_weight, key_weight)


def draw_w_query(key, part):
    return query_key_pair(key)[0].astype(jnp.bfloat16)


def draw_w_key(key, part):
    return query_key_pair(key)[1].astype(jnp.bfloat16)


def draw_conv_taps(key, part):
    random_split_keys = jax.random.split(jax.random.fold_in(key, 23), 1)
    sequence_positions = jnp.arange(CONV, dtype=jnp.float32) / (CONV - 1)
    raw_taps = jnp.clip(jax.random.normal(random_split_keys[0], (KERNEL, CONV), jnp.float32), -4.0, 4.0)
    channel_ramp = 10.0 ** (sequence_positions - 0.5)
    return raw_taps * KERNEL ** (-0.5) * channel_ramp[None, :]


def draw_cum_gate(key, part):
    random_split_keys = jax.random.split(jax.random.fold_in(key, 37), 7)
    head_order = jax.random.permutation(random_split_keys[0], HEAD_COUNT)
    slow_count = HEAD_COUNT // 2
    slow_heads = (head_order < slow_count)[:, None]
    slow_total = jax.random.uniform(random_split_keys[1], (HEAD_COUNT, 1), jnp.float32, 0.5, 1.0)
    fast_rate = 1.0 / jax.random.uniform(random_split_keys[2], (HEAD_COUNT, 1), jnp.float32, 30.0, 100.0)
    baseline_forget_rate = jnp.where(slow_heads, slow_total / TOKEN_COUNT, fast_rate)
    block_multiplier = jnp.exp(jax.random.uniform(random_split_keys[3], (HEAD_COUNT, N_SP), jnp.float32, math.log(0.5), math.log(2.0)))
    block_multiplier = jnp.repeat(block_multiplier, TOK_DEV, axis=1)
    roughness_multiplier = jax.random.uniform(random_split_keys[4], (HEAD_COUNT, TOKEN_COUNT), jnp.float32, 0.2, 1.8)
    spike_location = jax.random.randint(random_split_keys[5], (HEAD_COUNT, 2), 0, TOKEN_COUNT)
    spike_penalty = -jnp.log(jax.random.uniform(random_split_keys[6], (HEAD_COUNT, 2), jnp.float32, 0.6, 0.8))
    sequence_positions = jnp.arange(TOKEN_COUNT, dtype=jnp.int32)
    spike_events = jnp.sum(jnp.where(sequence_positions[None, None, :] == spike_location[:, :, None], spike_penalty[:, :, None], 0.0), axis=1)
    forget_rate_grid = baseline_forget_rate * block_multiplier * roughness_multiplier + spike_events
    return -jnp.cumsum(forget_rate_grid, axis=1)


def shard_levels(rng, dims, cuts, low, largest):
    gain = 1.0
    for axis_at, shards_of in cuts:
        draws = jax.random.uniform(jax.random.fold_in(jax.random.fold_in(rng, 6), axis_at), (shards_of,), jnp.float32, low / len(cuts), largest / len(cuts))
        gain = gain * jnp.repeat(jnp.exp(draws), dims[axis_at] // shards_of).reshape((-1,) + (1,) * (len(dims) - 1 - axis_at))
    return gain


def centred(key, dims, scale, bound, cuts=(), kind=jnp.bfloat16):
    drawn = scale * jax.random.normal(key, dims, jnp.float32)
    if cuts:
        drawn = drawn * shard_levels(key, dims, cuts, -0.22, 0.18)
    return jnp.clip(drawn, -bound, bound).astype(kind)


def setup_inputs(seed: int = 0) -> dict:
    seeds = jax.random.split(jax.random.key(seed), 13)
    tokens = centred(seeds[0], (TOKEN_COUNT, D), 1.0, 6.0, ((0, 32),))
    norm_gain = jnp.clip(1.0 + 0.18 * jax.random.normal(seeds[1], (D,), jnp.float32), 0.1, 1.9)
    w_query = draw_w_query(jax.random.fold_in(seeds[12], 71), 0)
    w_key = draw_w_key(jax.random.fold_in(seeds[12], 71), 0)
    w_value = centred(seeds[4], (D, ATT_WIDTH), D ** -0.5, 0.125, ((1, 4),))
    conv_in = centred(seeds[5], (D, CONV), D ** -0.5, 0.125, ((1, 4),))
    conv_gate = centred(seeds[6], (D, CONV), D ** -0.5, 0.125, ((1, 4),))
    conv_taps = draw_conv_taps(jax.random.fold_in(seeds[12], 71), 0)
    conv_gain = jnp.clip(1.0 + 0.18 * jax.random.normal(seeds[8], (CONV,), jnp.float32), 0.1, 1.9)
    cum_gate = draw_cum_gate(jax.random.fold_in(seeds[12], 71), 0)
    out_attn = centred(seeds[10], (ATT_WIDTH, D), (ATT_WIDTH // 16) ** -0.5, 0.75, ((0, 4),))
    out_conv = centred(seeds[11], (CONV, D), CONV ** -0.5, 0.125, ((0, 4),))
    return dict(tokens=tokens, norm_gain=norm_gain, w_query=w_query, w_key=w_key, w_value=w_value, conv_in=conv_in, conv_gate=conv_gate, conv_taps=conv_taps, conv_gain=conv_gain, cum_gate=cum_gate, out_attn=out_attn, out_conv=out_conv)


def by_heads(matrix):
    return matrix.reshape(TOKEN_COUNT, HEAD_COUNT, HEAD).transpose(1, 0, 2)

def head_attention(operands):
    query_head, key_head, value_head, cum_head = operands
    key_place = jnp.arange(TOKEN_COUNT, dtype=jnp.int32)

    def one_block(block_index):
        begin_row = (block_index * TOK_DEV).astype(jnp.int32)
        query_block = lax.dynamic_slice_in_dim(query_head, begin_row, TOK_DEV, 0)
        cum_block = lax.dynamic_slice_in_dim(cum_head, begin_row, TOK_DEV, 0)
        query_place = begin_row + jnp.arange(TOK_DEV, dtype=jnp.int32)
        scores = jnp.dot(query_block, key_head.T, preferred_element_type=jnp.float32)
        scores = scores + cum_block[:, None] - cum_head[None, :]
        visible = key_place[None, :] <= query_place[:, None]
        scores = jnp.where(visible, scores, -1e+30)
        row_max = lax.optimization_barrier(jnp.max(scores, axis=1))
        weights = jnp.where(visible, jnp.exp(scores - row_max[:, None]), 0.0)
        row_sum = lax.optimization_barrier(jnp.sum(weights, axis=1))
        result = jnp.dot(weights.astype(jnp.bfloat16), value_head, preferred_element_type=jnp.float32)
        result = (result / row_sum[:, None]).astype(jnp.bfloat16)
        return (result, row_max + jnp.log(row_sum))
    blocks_out, totals = lax.map(one_block, jnp.arange(N_SP, dtype=jnp.int32))
    return (blocks_out.reshape(TOKEN_COUNT, HEAD), totals.reshape(TOKEN_COUNT))

def reference(tokens, norm_gain, w_query, w_key, w_value, conv_in, conv_gate, conv_taps, conv_gain, cum_gate, out_attn, out_conv):
    wide = tokens.astype(jnp.float32)
    normed = (wide * lax.rsqrt(lax.optimization_barrier(jnp.mean(wide * wide, axis=1, keepdims=True)) + 1e-06) * norm_gain[None, :]).astype(jnp.bfloat16)
    query = (jnp.dot(normed, w_query, preferred_element_type=jnp.float32) * HEAD ** (-0.5)).astype(jnp.bfloat16)
    keyed = jnp.dot(normed, w_key, preferred_element_type=jnp.float32).astype(jnp.bfloat16)
    valued = jnp.dot(normed, w_value, preferred_element_type=jnp.float32).astype(jnp.bfloat16)
    attended, log_total = lax.map(head_attention, (by_heads(query), by_heads(keyed), by_heads(valued), cum_gate))
    attended = attended.transpose(1, 0, 2).reshape(TOKEN_COUNT, ATT_WIDTH)
    opened = jnp.dot(normed, conv_in, preferred_element_type=jnp.float32)
    gating = jnp.dot(normed, conv_gate, preferred_element_type=jnp.float32)
    gated = (opened * jax.nn.sigmoid(gating)).astype(jnp.bfloat16)
    padded = jnp.concatenate([jnp.zeros((KERNEL - 1, CONV), jnp.bfloat16), gated], axis=0).astype(jnp.float32)
    convolved = jnp.zeros((TOKEN_COUNT, CONV), jnp.float32)
    for tap_index in range(KERNEL):
        convolved = convolved + conv_taps[tap_index][None, :] * padded[tap_index:tap_index + TOKEN_COUNT]
    channel_square = lax.optimization_barrier(jnp.mean(convolved * convolved, axis=1, keepdims=True))
    conv_out = jax.nn.silu(convolved * lax.rsqrt(channel_square + 1e-06) * conv_gain[None, :]).astype(jnp.bfloat16)
    group_att = ATT_WIDTH // N_TP
    group_conv = CONV // N_TP
    mixed = jnp.zeros((TOKEN_COUNT, D), jnp.float32)
    for group in range(N_TP):
        group_part = jnp.dot(attended[:, group * group_att:(group + 1) * group_att], out_attn[group * group_att:(group + 1) * group_att], preferred_element_type=jnp.float32)
        group_part = group_part + jnp.dot(conv_out[:, group * group_conv:(group + 1) * group_conv], out_conv[group * group_conv:(group + 1) * group_conv], preferred_element_type=jnp.float32)
        group_part = lax.optimization_barrier(group_part.astype(jnp.bfloat16)).astype(jnp.float32)
        mixed = mixed + group_part
    return (mixed.astype(jnp.bfloat16), log_total)
```

```python
import functools

import jax
import jax.numpy as jnp
from jax import lax
from jax.experimental import pallas as pl
from jax.experimental.pallas import tpu as pltpu
from jax.sharding import PartitionSpec as P

HEAD = 64
CORES = 2


def attend_kernel(count, first, last, heads, idx_ref, q_ref, cum_ref, *refs):
    kv_refs = refs[:count]
    refs = refs[count:]
    if not first:
        m_in, l_in, a_in = refs[:3]
        refs = refs[3:]
    if last:
        out_ref, log_ref, m_ref, l_ref, a_ref = refs
    else:
        m_ref, l_ref, a_ref = refs
    rows = q_ref.shape[0]
    if not first:
        m_ref[...] = m_in[...]
        l_ref[...] = l_in[...]
        a_ref[...] = a_in[...]

    def visit(kv_ref, place, diagonal):
        start = pl.multiple_of(place * rows, rows)
        cum_cols = jnp.transpose(cum_ref[:, pl.ds(start, rows)])
        for h in range(heads):
            lo, hi = h * HEAD, (h + 1) * HEAD
            key = kv_ref[:, lo:hi]
            value = kv_ref[:, heads * HEAD + lo : heads * HEAD + hi]
            scores = lax.dot_general(
                key, q_ref[:, lo:hi], (((1,), (1,)), ((), ())), preferred_element_type=jnp.float32
            )
            scores = scores - cum_cols[:, h : h + 1]
            if diagonal:
                key_place = lax.broadcasted_iota(jnp.int32, scores.shape, 0)
                query_place = lax.broadcasted_iota(jnp.int32, scores.shape, 1)
                scores = jnp.where(key_place <= query_place, scores, -1e30)
            best = jnp.max(scores, axis=0, keepdims=True)
            if not diagonal:
                old = m_ref[h : h + 1, :]
                best = jnp.maximum(best, old)
                shrink = jnp.exp(old - best)
            weights = jnp.exp(scores - best)
            total = jnp.sum(weights, axis=0, keepdims=True)
            part = lax.dot_general(
                value,
                weights.astype(jnp.bfloat16),
                (((0,), (0,)), ((), ())),
                preferred_element_type=jnp.float32,
            )
            m_ref[h : h + 1, :] = best
            if diagonal:
                l_ref[h : h + 1, :] = total
                a_ref[lo:hi, :] = part
            else:
                l_ref[h : h + 1, :] = shrink * l_ref[h : h + 1, :] + total
                a_ref[lo:hi, :] = shrink * a_ref[lo:hi, :] + part

    if first:
        visit(kv_refs[0], idx_ref[0], True)
    else:
        for n in range(count):
            @pl.when(idx_ref[n] >= 0)
            def _(n=n):
                visit(kv_refs[n], idx_ref[n], False)

    if last:
        own = pl.multiple_of(idx_ref[count] * rows, rows)
        for h in range(heads):
            lo, hi = h * HEAD, (h + 1) * HEAD
            a_ref[lo:hi, :] = a_ref[lo:hi, :] / l_ref[h : h + 1, :]
        out_ref[...] = jnp.transpose(a_ref[...]).astype(jnp.bfloat16)
        log_ref[...] = m_ref[...] + jnp.log(l_ref[...]) + cum_ref[:, pl.ds(own, rows)][:heads]


def attend(query, cum, places, blocks, state, first, last, heads):
    rows, width = query.shape
    vmem = pl.BlockSpec(memory_space=pltpu.VMEM)
    stat = jax.ShapeDtypeStruct((heads, rows), jnp.float32)
    accum = jax.ShapeDtypeStruct((width, rows), jnp.float32)
    if last:
        out_shape = (jax.ShapeDtypeStruct((rows, width), jnp.bfloat16), stat)
        scratch = [pltpu.VMEM(stat.shape, stat.dtype)] * 2 + [pltpu.VMEM(accum.shape, accum.dtype)]
    else:
        out_shape = (stat, stat, accum)
        scratch = []
    operands = (query, cum) + tuple(blocks) + tuple(state)
    flops = 4 * rows * rows * width * len(blocks)
    return pl.pallas_call(
        functools.partial(attend_kernel, len(blocks), first, last, heads),
        out_shape=out_shape,
        in_specs=[pl.BlockSpec(memory_space=pltpu.SMEM)] + [vmem] * len(operands),
        out_specs=(vmem,) * len(out_shape),
        scratch_shapes=scratch,
        cost_estimate=pl.CostEstimate(
            flops=flops * 4, bytes_accessed=8 * rows * width, transcendentals=rows * rows * heads
        ),
        name="attend",
    )(jnp.stack(places).astype(jnp.int32), *operands)


def per_device(
    span_x,
    tokens,
    norm_gain,
    w_query,
    w_key,
    w_value,
    conv_in,
    conv_gate,
    conv_taps,
    conv_gain,
    cum_gate,
    out_attn,
    out_conv,
):
    width_att = w_query.shape[1]
    heads = width_att // HEAD
    channels = conv_in.shape[1]
    kernel_len = conv_taps.shape[0]
    n_tp, n_sp = lax.axis_size("tp"), lax.axis_size("sp")
    n_y, n_z = n_tp // CORES, n_sp // span_x
    tp_at, sp_at = lax.axis_index("tp"), lax.axis_index("sp")
    y_at, core_at = tp_at // CORES, tp_at % CORES
    z_at, x_at = sp_at // span_x, sp_at % span_x

    def swap_core(array):
        return lax.ppermute(array, "tp", [(i, i ^ 1) for i in range(n_tp)])

    def turn_y(array, by):
        return lax.ppermute(array, "tp", [(i, (i + by * CORES) % n_tp) for i in range(n_tp)])

    piece = tokens.shape[0]
    local_rows = piece * n_tp
    arrived = [tokens] + [turn_y(tokens, by) for by in range(1, n_y)]
    wide = jnp.zeros((local_rows, tokens.shape[1]), tokens.dtype)
    for by, block in enumerate(arrived):
        other = swap_core(block)
        base = ((y_at - by) % n_y) * CORES
        wide = lax.dynamic_update_slice_in_dim(wide, block, (base + core_at) * piece, 0)
        wide = lax.dynamic_update_slice_in_dim(wide, other, (base + 1 - core_at) * piece, 0)
    wide = wide.astype(jnp.float32)
    factor = lax.rsqrt(jnp.mean(wide * wide, axis=1, keepdims=True) + 1e-06)
    normed = (wide * factor * norm_gain[None, :]).astype(jnp.bfloat16)
    keyed = jnp.dot(normed, w_key, preferred_element_type=jnp.float32).astype(jnp.bfloat16)
    valued = jnp.dot(normed, w_value, preferred_element_type=jnp.float32).astype(jnp.bfloat16)
    own_kv = jnp.concatenate([keyed, valued], axis=1)

    chain = [own_kv]
    for k in range(1, n_z):
        pairs = [(s, s + span_x) for s in range(n_sp - span_x) if s // span_x >= k - 1]
        chain.append(lax.ppermute(chain[-1], "sp", pairs))
    handed = []
    for k in range(n_z):
        row = []
        for dx in range(1, span_x):
            pairs = []
            for s in range(n_sp):
                to = (s % span_x + dx) % span_x
                if s // span_x >= k and (k > 0 or to > s % span_x):
                    pairs.append((s, s // span_x * span_x + to))
            row.append(lax.ppermute(chain[k], "sp", pairs))
        handed.append(row)

    def place_of(k, dx):
        from_x = (x_at - dx) % span_x
        ok = z_at >= k
        if k == 0:
            ok = jnp.logical_and(ok, dx <= x_at)
        return jnp.where(ok, (z_at - k) * span_x + from_x, -1)

    query = (jnp.dot(normed, w_query, preferred_element_type=jnp.float32) * HEAD ** (-0.5)).astype(
        jnp.bfloat16
    )
    opened = jnp.dot(normed, conv_in, preferred_element_type=jnp.float32)
    gating = jnp.dot(normed, conv_gate, preferred_element_type=jnp.float32)
    gated = (opened * jax.nn.sigmoid(gating)).astype(jnp.bfloat16)

    rim_pairs = [(i, i + 1) for i in range(n_sp - 1)]
    rim_rows = lax.ppermute(gated[local_rows - (kernel_len - 1) :], "sp", rim_pairs)
    padded = jnp.concatenate([rim_rows, gated], axis=0).astype(jnp.float32)
    convolved = jnp.zeros((local_rows, channels), jnp.float32)
    for tap_index in range(kernel_len):
        convolved = (
            convolved + conv_taps[tap_index][None, :] * padded[tap_index : tap_index + local_rows]
        )
    square = jnp.sum(convolved * convolved, axis=1)
    square = square + swap_core(square)
    total_square = square
    for by in range(1, n_y):
        total_square = total_square + turn_y(square, by)
    channel_square = total_square / (channels * n_tp)
    conv_out = jax.nn.silu(
        convolved * lax.rsqrt(channel_square + 1e-06)[:, None] * conv_gain[None, :]
    ).astype(jnp.bfloat16)

    cum = jnp.pad(cum_gate, ((0, -heads % 8), (0, 0)))
    state = attend(query, cum, [sp_at], [own_kv], (), True, False, heads)
    for k in range(1, n_z + 1):
        last = k == n_z
        places = [place_of(k - 1, dx) for dx in range(1, span_x)]
        blocks = list(handed[k - 1])
        if not last:
            places.append(place_of(k, 0))
            blocks.append(chain[k])
        state = attend(query, cum, places + [sp_at], blocks, state, False, last, heads)
    attended, log_total = state

    group_part = jnp.dot(attended, out_attn, preferred_element_type=jnp.float32)
    group_part = group_part + jnp.dot(conv_out, out_conv, preferred_element_type=jnp.float32)
    group_part = group_part.astype(jnp.bfloat16).reshape(n_y, CORES, piece, -1)
    keep = lax.dynamic_index_in_dim(group_part, core_at, 1, keepdims=False)
    give = lax.dynamic_index_in_dim(group_part, 1 - core_at, 1, keepdims=False)
    both = keep.astype(jnp.float32) + swap_core(give).astype(jnp.float32)
    mixed = lax.dynamic_index_in_dim(both, y_at, 0, keepdims=False)
    for by in range(1, n_y):
        leaving = lax.dynamic_index_in_dim(both, (y_at + by) % n_y, 0, keepdims=False)
        mixed = mixed + turn_y(leaving.astype(jnp.bfloat16), by).astype(jnp.float32)
    return (mixed.astype(jnp.bfloat16), log_total)


def solution(mesh):
    column = [getattr(d, "coords", None) for d in mesh.devices[:, 0].flat]
    span_x = 2 if column[0] is None else len({c[0] for c in column})
    in_specs = (
        P(("sp", "tp"), None),
        P(),
        P(None, "tp"),
        P(None, "tp"),
        P(None, "tp"),
        P(None, "tp"),
        P(None, "tp"),
        P(None, "tp"),
        P("tp"),
        P("tp", None),
        P("tp", None),
        P("tp", None),
    )
    out_specs = (P(("sp", "tp"), None), P("tp", "sp"))
    return jax.shard_map(
        functools.partial(per_device, span_x),
        mesh=mesh,
        in_specs=in_specs,
        out_specs=out_specs,
        check_vma=False,
    )
```

```python
import functools

import jax
import jax.numpy as jnp
from jax import lax
from jax.experimental import pallas as pl
from jax.experimental.pallas import tpu as pltpu
from jax.sharding import PartitionSpec as P

HEAD = 64
CORES = 2


def attend_kernel(count, first, last, heads, idx_ref, q_ref, cum_ref, *refs):
    kv_refs = refs[:count]
    refs = refs[count:]
    if not first:
        m_in, l_in, a_in = refs[:3]
        refs = refs[3:]
    if last:
        out_ref, log_ref, m_ref, l_ref, a_ref = refs
    else:
        m_ref, l_ref, a_ref = refs
    rows = q_ref.shape[0]
    if not first:
        m_ref[...] = m_in[...]
        l_ref[...] = l_in[...]
        a_ref[...] = a_in[...]

    def visit(kv_ref, place, diagonal):
        start = pl.multiple_of(place * rows, rows)
        cum_cols = jnp.transpose(cum_ref[:, pl.ds(start, rows)])
        for h in range(heads):
            lo, hi = h * HEAD, (h + 1) * HEAD
            key = kv_ref[:, lo:hi]
            value = kv_ref[:, heads * HEAD + lo : heads * HEAD + hi]
            scores = lax.dot_general(
                key, q_ref[:, lo:hi], (((1,), (1,)), ((), ())), preferred_element_type=jnp.float32
            )
            scores = scores - cum_cols[:, h : h + 1]
            if diagonal:
                key_place = lax.broadcasted_iota(jnp.int32, scores.shape, 0)
                query_place = lax.broadcasted_iota(jnp.int32, scores.shape, 1)
                scores = jnp.where(key_place <= query_place, scores, -1e30)
            best = jnp.max(scores, axis=0, keepdims=True)
            if not diagonal:
                old = m_ref[h : h + 1, :]
                best = jnp.maximum(best, old)
                shrink = jnp.exp(old - best)
            weights = jnp.exp(scores - best)
            total = jnp.sum(weights, axis=0, keepdims=True)
            part = lax.dot_general(
                value,
                weights.astype(jnp.bfloat16),
                (((0,), (0,)), ((), ())),
                preferred_element_type=jnp.float32,
            )
            m_ref[h : h + 1, :] = best
            if diagonal:
                l_ref[h : h + 1, :] = total
                a_ref[lo:hi, :] = part
            else:
                l_ref[h : h + 1, :] = shrink * l_ref[h : h + 1, :] + total
                a_ref[lo:hi, :] = shrink * a_ref[lo:hi, :] + part

    if first:
        visit(kv_refs[0], idx_ref[0], True)
    else:
        for n in range(count):
            @pl.when(idx_ref[n] >= 0)
            def _(n=n):
                visit(kv_refs[n], idx_ref[n], False)

    if last:
        own = pl.multiple_of(idx_ref[count] * rows, rows)
        for h in range(heads):
            lo, hi = h * HEAD, (h + 1) * HEAD
            a_ref[lo:hi, :] = a_ref[lo:hi, :] / l_ref[h : h + 1, :]
        out_ref[...] = jnp.transpose(a_ref[...]).astype(jnp.bfloat16)
        log_ref[...] = m_ref[...] + jnp.log(l_ref[...]) + cum_ref[:, pl.ds(own, rows)][:heads]


def attend(query, cum, places, blocks, state, first, last, heads):
    rows, width = query.shape
    vmem = pl.BlockSpec(memory_space=pltpu.VMEM)
    stat = jax.ShapeDtypeStruct((heads, rows), jnp.float32)
    accum = jax.ShapeDtypeStruct((width, rows), jnp.float32)
    if last:
        out_shape = (jax.ShapeDtypeStruct((rows, width), jnp.bfloat16), stat)
        scratch = [pltpu.VMEM(stat.shape, stat.dtype)] * 2 + [pltpu.VMEM(accum.shape, accum.dtype)]
    else:
        out_shape = (stat, stat, accum)
        scratch = []
    operands = (query, cum) + tuple(blocks) + tuple(state)
    flops = 4 * rows * rows * width * len(blocks)
    return pl.pallas_call(
        functools.partial(attend_kernel, len(blocks), first, last, heads),
        out_shape=out_shape,
        in_specs=[pl.BlockSpec(memory_space=pltpu.SMEM)] + [vmem] * len(operands),
        out_specs=(vmem,) * len(out_shape),
        scratch_shapes=scratch,
        cost_estimate=pl.CostEstimate(
            flops=flops * 4, bytes_accessed=8 * rows * width, transcendentals=rows * rows * heads
        ),
        name="attend",
    )(jnp.stack(places).astype(jnp.int32), *operands)


def per_device(
    span_x,
    tokens,
    norm_gain,
    w_query,
    w_key,
    w_value,
    conv_in,
    conv_gate,
    conv_taps,
    conv_gain,
    cum_gate,
    out_attn,
    out_conv,
):
    width_att = w_query.shape[1]
    heads = width_att // HEAD
    channels = conv_in.shape[1]
    kernel_len = conv_taps.shape[0]
    n_tp, n_sp = lax.axis_size("tp"), lax.axis_size("sp")
    n_y, n_z = n_tp // CORES, n_sp // span_x
    tp_at, sp_at = lax.axis_index("tp"), lax.axis_index("sp")
    y_at, core_at = tp_at // CORES, tp_at % CORES
    z_at, x_at = sp_at // span_x, sp_at % span_x

    def swap_core(array):
        return lax.ppermute(array, "tp", [(i, i ^ 1) for i in range(n_tp)])

    def turn_y(array, by):
        return lax.ppermute(array, "tp", [(i, (i + by * CORES) % n_tp) for i in range(n_tp)])

    piece = tokens.shape[0]
    local_rows = piece * n_tp
    arrived = [tokens] + [turn_y(tokens, by) for by in range(1, n_y)]
    wide = jnp.zeros((local_rows, tokens.shape[1]), tokens.dtype)
    for by, block in enumerate(arrived):
        other = swap_core(block)
        base = ((y_at - by) % n_y) * CORES
        wide = lax.dynamic_update_slice_in_dim(wide, block, (base + core_at) * piece, 0)
        wide = lax.dynamic_update_slice_in_dim(wide, other, (base + 1 - core_at) * piece, 0)
    wide = wide.astype(jnp.float32)
    factor = lax.rsqrt(jnp.mean(wide * wide, axis=1, keepdims=True) + 1e-06)
    normed = (wide * factor * norm_gain[None, :]).astype(jnp.bfloat16)
    keyed = jnp.dot(normed, w_key, preferred_element_type=jnp.float32).astype(jnp.bfloat16)
    valued = jnp.dot(normed, w_value, preferred_element_type=jnp.float32).astype(jnp.bfloat16)
    own_kv = jnp.concatenate([keyed, valued], axis=1)

    chain = [own_kv]
    for k in range(1, n_z):
        pairs = [(s, s + span_x) for s in range(n_sp - span_x) if s // span_x >= k - 1]
        chain.append(lax.ppermute(chain[-1], "sp", pairs))
    handed = []
    for k in range(n_z):
        row = []
        for dx in range(1, span_x):
            pairs = []
            for s in range(n_sp):
                to = (s % span_x + dx) % span_x
                if s // span_x >= k and (k > 0 or to > s % span_x):
                    pairs.append((s, s // span_x * span_x + to))
            row.append(lax.ppermute(chain[k], "sp", pairs))
        handed.append(row)

    def place_of(k, dx):
        from_x = (x_at - dx) % span_x
        ok = z_at >= k
        if k == 0:
            ok = jnp.logical_and(ok, dx <= x_at)
        return jnp.where(ok, (z_at - k) * span_x + from_x, -1)

    query = (jnp.dot(normed, w_query, preferred_element_type=jnp.float32) * HEAD ** (-0.5)).astype(
        jnp.bfloat16
    )
    opened = jnp.dot(normed, conv_in, preferred_element_type=jnp.float32)
    gating = jnp.dot(normed, conv_gate, preferred_element_type=jnp.float32)
    gated = (opened * jax.nn.sigmoid(gating)).astype(jnp.bfloat16)

    rim_pairs = [(i, i + 1) for i in range(n_sp - 1)]
    rim_rows = lax.ppermute(gated[local_rows - (kernel_len - 1) :], "sp", rim_pairs)
    padded = jnp.concatenate([rim_rows, gated], axis=0).astype(jnp.float32)
    convolved = jnp.zeros((local_rows, channels), jnp.float32)
    for tap_index in range(kernel_len):
        convolved = (
            convolved + conv_taps[tap_index][None, :] * padded[tap_index : tap_index + local_rows]
        )
    square = jnp.sum(convolved * convolved, axis=1)
    square = square + swap_core(square)
    total_square = square
    for by in range(1, n_y):
        total_square = total_square + turn_y(square, by)
    channel_square = total_square / (channels * n_tp)
    conv_out = jax.nn.silu(
        convolved * lax.rsqrt(channel_square + 1e-06)[:, None] * conv_gain[None, :]
    ).astype(jnp.bfloat16)

    cum = jnp.pad(cum_gate, ((0, -heads % 8), (0, 0)))
    state = attend(query, cum, [sp_at], [own_kv], (), True, False, heads)
    for k in range(1, n_z + 1):
        last = k == n_z
        places = [place_of(k - 1, dx) for dx in range(1, span_x)]
        blocks = list(handed[k - 1])
        if not last:
            places.append(place_of(k, 0))
            blocks.append(chain[k])
        state = attend(query, cum, places + [sp_at], blocks, state, False, last, heads)
    attended, log_total = state

    group_part = jnp.dot(attended, out_attn, preferred_element_type=jnp.float32)
    group_part = group_part + jnp.dot(conv_out, out_conv, preferred_element_type=jnp.float32)
    group_part = group_part.astype(jnp.bfloat16).reshape(n_y, CORES, piece, -1)
    def pick(array, at):
        chosen = array[0]
        for n in range(1, array.shape[0]):
            chosen = jnp.where(at == n, array[n], chosen)
        return chosen

    keep = jnp.where(core_at == 0, group_part[:, 0], group_part[:, 1])
    give = jnp.where(core_at == 0, group_part[:, 1], group_part[:, 0])
    both = keep.astype(jnp.float32) + swap_core(give).astype(jnp.float32)
    mixed = pick(both, y_at)
    for by in range(1, n_y):
        leaving = pick(both, (y_at + by) % n_y)
        mixed = mixed + turn_y(leaving.astype(jnp.bfloat16), by).astype(jnp.float32)
    return (mixed.astype(jnp.bfloat16), log_total)


def solution(mesh):
    column = [getattr(d, "coords", None) for d in mesh.devices[:, 0].flat]
    span_x = 2 if column[0] is None else len({c[0] for c in column})
    in_specs = (
        P(("sp", "tp"), None),
        P(),
        P(None, "tp"),
        P(None, "tp"),
        P(None, "tp"),
        P(None, "tp"),
        P(None, "tp"),
        P(None, "tp"),
        P("tp"),
        P("tp", None),
        P("tp", None),
        P("tp", None),
    )
    out_specs = (P(("sp", "tp"), None), P("tp", "sp"))
    return jax.shard_map(
        functools.partial(per_device, span_x),
        mesh=mesh,
        in_specs=in_specs,
        out_specs=out_specs,
        check_vma=False,
    )
```
